32 devices in a mesh: fs: 8 (over z, y), tp: 4 (over x, core).
Axes of the slice: x: 2, y: 2, z: 4, core: 2. Of those that a mesh axis runs over, the one named last changes fastest.
Arguments:
- saved_inputs: bfloat16 [4096, 3072], P('fs'), may hold values from -6 to 6
- query_cotangent: bfloat16 [4096, 3072], P('fs', 'tp'), may hold values from -0.75 to 0.75
- attn_outputs: bfloat16 [4096, 3072], P('fs', 'tp'), may hold values from -6 to 6
- out_cotangent: bfloat16 [4096, 3072], P('fs'), may hold values from -0.75 to 0.75
- left_factor: bfloat16 [3072, 384], P('fs', 'tp'), may hold values from -0.109375 to 0.109375
- right_factor: bfloat16 [3072, 384], P('fs', 'tp'), may hold values from -0.109375 to 0.109375
- query_master: float32 [3072, 3072], P('fs', 'tp'), may hold values from -0.109375 to 0.109375
- out_master: float32 [3072, 3072], P('tp', 'fs'), may hold values from -0.109375 to 0.109375
- first_moment: float32 [2, 384, 3072], P(None, 'fs', 'tp'), may hold values from -14 to 14
- second_moment: float32 [2, 384, 3072], P(None, 'fs', 'tp'), may hold values from 0.3 to 3
Outputs:
- query_new: float32 [3072, 3072], P('fs', 'tp')
- out_new: float32 [3072, 3072], P('tp', 'fs')
- query_copy: bfloat16 [3072, 3072], P(None, 'tp')
- out_copy: bfloat16 [3072, 3072], P('tp')
- first_new: float32 [2, 384, 3072], P(None, 'fs', 'tp')
- second_new: float32 [2, 384, 3072], P(None, 'fs', 'tp')
The draws below stay inside these ranges and needn't reach their ends.
All inputs are finite; a program needn't handle non-finite values.
Results may differ from the reference program's by a relative error of at most 0.0025.
Values may be sent and summed in bfloat16 or wider, within the bound.
A program may use at most 64 MiB of HBM per device.

```python
import math
import jax
import jax.numpy as jnp
from jax import lax

D = 3072
RANK = 384
QW = 3072
TOKENS = 4096


def draw_first_moment(key, part):
    row_pos = jnp.arange(RANK, dtype=jnp.float32) / RANK
    col_pos = jnp.arange(QW, dtype=jnp.float32) / QW
    base = jnp.clip(jax.random.normal(key, (2, RANK, QW), jnp.float32), -4.0, 4.0)
    growth = 3.0
    spread = growth ** row_pos[:, None] * growth ** col_pos[None, :] / growth
    return (base * spread[None]).astype(jnp.float32)


def shard_levels(own_key, extent, shards, least, high):
    gain = 1.0
    for position, blocks in shards:
        heights = jax.random.uniform(jax.random.fold_in(jax.random.fold_in(own_key, 6), position), (blocks,), jnp.float32, least / len(shards), high / len(shards))
        gain = gain * jnp.repeat(jnp.exp(heights), extent[position] // blocks).reshape((-1,) + (1,) * (len(extent) - 1 - position))
    return gain


def normal_values(own_key, dims, scale, reach, shards=(), held_as=jnp.bfloat16):
    drawn = jax.random.normal(own_key, dims, jnp.float32) * scale
    if len(shards) > 0:
        drawn = shard_levels(own_key, dims, shards, -0.22, 0.18) * drawn
    return jnp.clip(drawn, min=-reach, max=reach).astype(held_as)


def setup_inputs(seed: int = 0) -> dict:
    key_list = jax.random.split(jax.random.key(seed), 11)
    return {
        "saved_inputs": normal_values(key_list[0], (TOKENS, D), 1.0, 6.0, ((0, 8),)),
        "query_cotangent": normal_values(key_list[1], (TOKENS, QW), (8.0 / TOKENS ** 0.5), 0.75, ((0, 8), (1, 4))),
        "attn_outputs": normal_values(key_list[2], (TOKENS, QW), 1.0, 6.0, ((0, 8), (1, 4))),
        "out_cotangent": normal_values(key_list[3], (TOKENS, D), (8.0 / TOKENS ** 0.5), 0.75, ((0, 8),)),
        "left_factor": normal_values(key_list[4], (D, RANK), D ** -0.5, 0.109375, ((0, 8), (1, 4))),
        "right_factor": normal_values(key_list[5], (D, RANK), D ** -0.5, 0.109375, ((0, 8), (1, 4))),
        "query_master": normal_values(key_list[6], (D, QW), D ** -0.5, 0.109375, ((0, 8), (1, 4)), jnp.float32),
        "out_master": normal_values(key_list[7], (QW, D), QW ** -0.5, 0.109375, ((0, 4), (1, 8)), jnp.float32),
        "first_moment": draw_first_moment(jax.random.fold_in(key_list[10], 71), 0),
        "second_moment": jnp.clip(jnp.exp(math.log(3.0) - 2.3025851 * jax.random.uniform(key_list[9], (2, RANK, QW), jnp.float32) ** shard_levels(key_list[9], (2, RANK, QW), ((1, 8), (2, 4)), -0.2, 0.2)), 0.3, 3.0),
    }


def reference(saved_inputs, query_cotangent, attn_outputs, out_cotangent, left_factor, right_factor, query_master, out_master, first_moment, second_moment):
    left_proj = jnp.dot(saved_inputs, left_factor, preferred_element_type=jnp.float32).astype(jnp.bfloat16)
    right_proj = jnp.dot(out_cotangent, right_factor, preferred_element_type=jnp.float32).astype(jnp.bfloat16)
    grad_query = jnp.dot(left_proj.T, query_cotangent, preferred_element_type=jnp.float32)
    grad_output = jnp.dot(right_proj.T, attn_outputs, preferred_element_type=jnp.float32)
    grads = jnp.stack([grad_query, grad_output], axis=0)
    first_new = 0.9 * first_moment + 0.1 * grads
    second_new = 0.99 * second_moment + 0.01 * grads * grads
    direction = first_new / (jnp.sqrt(second_new) + 1e-08)
    scale = lax.rsqrt(lax.optimization_barrier(jnp.mean(direction * direction, axis=(1, 2))) + 1e-06)
    direction_low = direction.astype(jnp.bfloat16)
    step_query = scale[0] * jnp.dot(left_factor, direction_low[0], preferred_element_type=jnp.float32)
    step_output = scale[1] * jnp.dot(direction_low[1].T, right_factor.T, preferred_element_type=jnp.float32)
    query_new = query_master - 0.01 * step_query
    out_new = out_master - 0.01 * step_output
    return (query_new, out_new, query_new.astype(jnp.bfloat16), out_new.astype(jnp.bfloat16), first_new, second_new)
```

```python
import functools

import jax
import jax.numpy as jnp
from jax import lax
from jax.experimental import pallas as pl
from jax.experimental.pallas import tpu as pltpu
from jax.sharding import PartitionSpec as P

MESH = pl.DeviceIdType.MESH
PAIR = 2
MASTER_GAIN = 2.0**19
NT = (((1,), (1,)), ((), ()))
TN = (((0,), (0,)), ((), ()))


def moment_step(first, second, grads):
    first_next = 0.9 * first + 0.1 * grads
    second_next = 0.99 * second + 0.01 * grads * grads
    return (first_next, second_next, first_next / (jnp.sqrt(second_next) + 1e-08))


def rows(index, size):
    return pl.ds(pl.multiple_of(index * size, size), size)


def peer_along(axis, index):
    if axis == "fs":
        return (index, lax.axis_index("tp"))
    return (lax.axis_index("fs"), index)


class Gather:
    def __init__(self, axis, count, view, sems, own=None):
        self.axis, self.outer, self.view, self.sems = axis, count // PAIR, view, sems
        me = lax.axis_index(axis)
        self.high, self.low = me // PAIR, lax.rem(me, PAIR)
        self.own = view(me) if own is None else own
        self.me = me

    def copy(self, src, dst, stage, slot, target):
        return pltpu.make_async_remote_copy(
            src_ref=src,
            dst_ref=dst,
            send_sem=self.sems.at[stage, 0, slot],
            recv_sem=self.sems.at[stage, 1, slot],
            device_id=peer_along(self.axis, target),
            device_id_type=MESH,
        )

    def index(self, offset, low):
        return lax.rem(self.high + offset, self.outer) * PAIR + low

    def outward(self, offset):
        return self.copy(self.own, self.view(self.me), 0, offset, self.index(offset, self.low))

    def inward(self, offset):
        source = self.index(self.outer - offset, self.low)
        src = self.own if offset == 0 else self.view(source)
        partner = self.high * PAIR + 1 - self.low
        return self.copy(src, self.view(self.me if offset == 0 else source), 1, offset, partner)

    def start(self):
        for offset in range(self.outer - 1, 0, -1):
            self.outward(offset).start()
        self.inward(0).start()

    def forward(self):
        for offset in range(1, self.outer):
            self.outward(offset).wait_recv()
            self.inward(offset).start()

    def finish(self):
        for offset in range(self.outer):
            self.inward(offset).wait_recv()
        for offset in range(1, self.outer):
            self.outward(offset).wait_send()
        for offset in range(self.outer):
            self.inward(offset).wait_send()


def kernel(
    n_fs,
    n_tp,
    saved_hbm,
    outcot_hbm,
    querycot_hbm,
    attn_hbm,
    factor_ref,
    first_ref,
    second_ref,
    factors_ref,
    dirs_ref,
    first_out,
    second_out,
    square_out,
    saved,
    outcot,
    querycot,
    attn,
    proj,
    grad,
    pair_send,
    pair_recv,
    far_send,
    far_recv,
    own_dir,
    square_buf,
    load_sems,
    factor_sems,
    proj_sems,
    columns_sems,
    pair_sems,
    far_sems,
    dir_sems,
    square_sems,
):
    me, column = lax.axis_index("fs"), lax.axis_index("tp")
    high, low = me // PAIR, lax.rem(me, PAIR)
    outer = n_fs // PAIR
    part = factor_ref.shape[1]
    width = factor_ref.shape[2]
    depth = first_ref.shape[1]
    loads = [
        pltpu.make_async_copy(src, dst, load_sems.at[i])
        for i, (src, dst) in enumerate(
            ((saved_hbm, saved), (outcot_hbm, outcot), (querycot_hbm, querycot), (attn_hbm, attn))
        )
    ]
    for load in loads:
        load.start()

    peers = [(lax.rem(high + i, outer) * PAIR + low, column) for i in range(1, outer)]
    peers.append((high * PAIR + 1 - low, column))
    peers += [(me, lax.rem(column + i, n_tp)) for i in range(1, n_tp)]
    barrier = pltpu.get_barrier_semaphore()
    for peer in peers:
        pl.semaphore_signal(barrier, inc=1, device_id=peer, device_id_type=MESH)
    pl.semaphore_wait(barrier, len(peers))

    factors = Gather(
        "fs",
        n_fs,
        lambda i: factors_ref.at[:, rows(column, part), rows(i, width)],
        factor_sems,
        own=factor_ref,
    )
    factors.start()
    factors_ref[:, rows(column, part), rows(me, width)] = factor_ref[...]
    factors.forward()
    factors.finish()

    gathers = []
    for k, tokens in enumerate((saved, outcot)):
        loads[k].wait()
        part_proj = lax.dot_general(
            factors_ref[k, rows(column, part), :],
            tokens[...],
            NT,
            preferred_element_type=jnp.float32,
        )
        proj[k, rows(column, part), :] = part_proj.astype(proj.dtype)
        gather = Gather(
            "tp", n_tp, lambda i, k=k: proj.at[k, rows(i, part), :], proj_sems.at[k]
        )
        gather.start()
        gathers.append(gather)
    columns = Gather("tp", n_tp, lambda i: factors_ref.at[:, rows(i, part), :], columns_sems)
    for gather in gathers:
        gather.forward()
    columns.start()
    for k, (gather, cot) in enumerate(zip(gathers, (querycot, attn))):
        gather.finish()
        loads[2 + k].wait()
        grad[k, :, :] = jnp.dot(proj[k], cot[...], preferred_element_type=jnp.float32)

    def pair_copy(offset):
        return pltpu.make_async_remote_copy(
            src_ref=pair_send.at[offset],
            dst_ref=pair_recv.at[offset],
            send_sem=pair_sems.at[0, offset],
            recv_sem=pair_sems.at[1, offset],
            device_id=(high * PAIR + 1 - low, column),
            device_id_type=MESH,
        )

    def far_copy(offset):
        return pltpu.make_async_remote_copy(
            src_ref=far_send.at[offset],
            dst_ref=far_recv.at[offset],
            send_sem=far_sems.at[0, offset],
            recv_sem=far_sems.at[1, offset],
            device_id=(lax.rem(high + offset, outer) * PAIR + low, column),
            device_id_type=MESH,
        )

    order = list(range(outer - 1, 0, -1)) + [0]
    for offset in order:
        target = lax.rem(high + offset, outer) * PAIR + 1 - low
        pair_send[offset] = grad[:, rows(target, depth), :].astype(pair_send.dtype)
        pair_copy(offset).start()
    for offset in order:
        target = lax.rem(high + offset, outer) * PAIR + low
        pair_copy(offset).wait_recv()
        both = grad[:, rows(target, depth), :] + pair_recv[offset].astype(jnp.float32)
        if offset:
            far_send[offset] = both.astype(far_send.dtype)
            far_copy(offset).start()
    total = both
    columns.forward()
    for offset in range(1, outer):
        far_copy(offset).wait_recv()
        total = total + far_recv[offset].astype(jnp.float32)

    first_new, second_new, direction = moment_step(first_ref[...], second_ref[...], total)
    own_dir[...] = direction.astype(own_dir.dtype)
    spread = Gather("fs", n_fs, lambda i: dirs_ref.at[:, rows(i, depth), :], dir_sems, own=own_dir)
    spread.start()
    dirs_ref[:, rows(me, depth), :] = own_dir[...]
    first_out[...] = first_new
    second_out[...] = second_new
    squares = direction * direction
    shape = square_out.shape
    row = lax.broadcasted_iota(jnp.int32, shape, 0)
    mine = jnp.where(row == 0, jnp.sum(squares[0]), jnp.sum(squares[1]))

    rounds = (
        [(me, lax.rem(column + i, n_tp)) for i in range(1, n_tp)],
        [(lax.rem(high + i, outer) * PAIR + low, column) for i in range(1, outer)],
        [(high * PAIR + 1 - low, column)],
    )
    slot = 0
    tiny = []
    for stage, targets in enumerate(rounds):
        square_buf[slot] = mine
        base = slot
        copies = []
        for target in targets:
            slot += 1
            copies.append(
                pltpu.make_async_remote_copy(
                    src_ref=square_buf.at[base],
                    dst_ref=square_buf.at[slot],
                    send_sem=square_sems.at[0, slot],
                    recv_sem=square_sems.at[1, slot],
                    device_id=target,
                    device_id_type=MESH,
                )
            )
        for copy in copies:
            copy.start()
        if stage == 1:
            spread.forward()
        for i, copy in enumerate(copies):
            copy.wait_recv()
            mine = mine + square_buf[base + 1 + i]
        tiny += copies
        slot += 1
    square_out[...] = mine
    spread.finish()
    columns.finish()
    for offset in order:
        pair_copy(offset).wait_send()
        if offset:
            far_copy(offset).wait_send()
    for copy in tiny:
        copy.wait_send()


def moment_kernel(n_fs, n_tp, saved_inputs, out_cotangent, query_cotangent, attn_outputs, factor, first, second):
    tokens, model = saved_inputs.shape
    features = query_cotangent.shape[1]
    part = factor.shape[1]
    depth = first.shape[1]
    rank = part * n_tp
    outer = n_fs // PAIR
    low = jnp.bfloat16
    vmem = pl.BlockSpec(memory_space=pltpu.VMEM)
    anywhere = pl.BlockSpec(memory_space=pl.ANY)
    dma = pltpu.SemaphoreType.DMA
    tiny_slots = n_tp + outer + PAIR
    return pl.pallas_call(
        functools.partial(kernel, n_fs, n_tp),
        out_shape=(
            jax.ShapeDtypeStruct((2, rank, model), low),
            jax.ShapeDtypeStruct((2, rank, features), low),
            jax.ShapeDtypeStruct(first.shape, jnp.float32),
            jax.ShapeDtypeStruct(first.shape, jnp.float32),
            jax.ShapeDtypeStruct((8, 128), jnp.float32),
        ),
        in_specs=[anywhere] * 4 + [vmem] * 3,
        out_specs=(vmem,) * 5,
        scratch_shapes=[
            pltpu.VMEM((tokens, model), low),
            pltpu.VMEM((tokens, model), low),
            pltpu.VMEM((tokens, features), low),
            pltpu.VMEM((tokens, features), low),
            pltpu.VMEM((2, rank, tokens), low),
            pltpu.VMEM((2, rank, features), jnp.float32),
            pltpu.VMEM((outer, 2, depth, features), low),
            pltpu.VMEM((outer, 2, depth, features), low),
            pltpu.VMEM((outer, 2, depth, features), low),
            pltpu.VMEM((outer, 2, depth, features), low),
            pltpu.VMEM((2, depth, features), low),
            pltpu.VMEM((tiny_slots, 8, 128), jnp.float32),
            dma((4,)),
            dma((2, 2, outer)),
            dma((2, 2, 2, n_tp // PAIR)),
            dma((2, 2, n_tp // PAIR)),
            dma((2, outer)),
            dma((2, outer)),
            dma((2, 2, outer)),
            dma((2, tiny_slots)),
        ],
        compiler_params=pltpu.CompilerParams(
            collective_id=0, has_side_effects=True, vmem_limit_bytes=48 * 2**20
        ),
        cost_estimate=pl.CostEstimate(
            flops=4 * tokens * rank * (model + features), bytes_accessed=200 * 2**20, transcendentals=0
        ),
    )(saved_inputs, out_cotangent, query_cotangent, attn_outputs, factor, first, second)


def fast_body(
    n_fs,
    n_tp,
    saved_inputs,
    query_cotangent,
    attn_outputs,
    out_cotangent,
    left_factor,
    right_factor,
    query_master,
    out_master,
    first_moment,
    second_moment,
):
    query_all = lax.all_gather(
        (query_master * MASTER_GAIN).astype(jnp.float16), "fs", axis=0, tiled=True
    )
    out_all = lax.all_gather(
        (out_master * MASTER_GAIN).astype(jnp.float16), "fs", axis=1, tiled=True
    )
    factor = jnp.stack([left_factor.T, right_factor.T])
    factors, dirs, first_new, second_new, squares = moment_kernel(
        n_fs,
        n_tp,
        saved_inputs,
        out_cotangent,
        query_cotangent,
        attn_outputs,
        factor,
        first_moment,
        second_moment,
    )
    rank, features = dirs.shape[1:]
    entries = rank * features * n_tp
    scale = 0.01 * lax.rsqrt(squares[:2, 0] / entries + 1e-06)
    width = left_factor.shape[0]
    start = lax.axis_index("fs") * width
    own = lax.dynamic_slice_in_dim(factors, start, width, axis=2)
    f32 = jnp.float32
    query_new = query_master - scale[0] * lax.dot_general(own[0], dirs[0], TN, preferred_element_type=f32)
    out_new = out_master - scale[1] * lax.dot_general(dirs[1], own[1], TN, preferred_element_type=f32)
    query_step = lax.dot_general(factors[0], dirs[0], TN, preferred_element_type=f32)
    out_step = lax.dot_general(dirs[1], factors[1], TN, preferred_element_type=f32)
    query_copy = (query_all.astype(f32) * (1 / MASTER_GAIN) - scale[0] * query_step).astype(jnp.bfloat16)
    out_copy = (out_all.astype(f32) * (1 / MASTER_GAIN) - scale[1] * out_step).astype(jnp.bfloat16)
    return (query_new, out_new, query_copy, out_copy, first_new, second_new)


def plain_body(
    saved_inputs,
    query_cotangent,
    attn_outputs,
    out_cotangent,
    left_factor,
    right_factor,
    query_master,
    out_master,
    first_moment,
    second_moment,
):
    left_part = jnp.dot(
        saved_inputs,
        lax.all_gather(left_factor, "fs", axis=0, tiled=True),
        preferred_element_type=jnp.float32,
    )
    right_part = jnp.dot(
        out_cotangent,
        lax.all_gather(right_factor, "fs", axis=0, tiled=True),
        preferred_element_type=jnp.float32,
    )
    left_proj, right_proj, left_rows, right_rows = (
        lax.all_gather(left_part.astype(jnp.bfloat16), "tp", axis=1, tiled=True),
        lax.all_gather(right_part.astype(jnp.bfloat16), "tp", axis=1, tiled=True),
        lax.all_gather(left_factor, "tp", axis=1, tiled=True),
        lax.all_gather(right_factor, "tp", axis=1, tiled=True),
    )
    depth = first_moment.shape[1]
    grad_query = lax.dot_general(left_proj, query_cotangent, TN, preferred_element_type=jnp.float32)
    grad_output = lax.dot_general(right_proj, attn_outputs, TN, preferred_element_type=jnp.float32)
    summed = lax.psum_scatter(
        jnp.stack([grad_query, grad_output], axis=1), "fs", scatter_dimension=0, tiled=True
    )
    grads = jnp.transpose(summed, (1, 0, 2))
    first_new, second_new, own_direction = moment_step(first_moment, second_moment, grads)
    direction_all = lax.all_gather(own_direction.astype(jnp.bfloat16), "fs", axis=1, tiled=True)
    squares = jnp.sum(own_direction * own_direction, axis=(1, 2))
    total = lax.psum(squares, ("fs", "tp"))
    entries = depth * lax.axis_size("fs") * own_direction.shape[2] * lax.axis_size("tp")
    scale = lax.rsqrt(total / entries + 1e-06)
    step_query = scale[0] * jnp.dot(left_rows, direction_all[0], preferred_element_type=jnp.float32)
    step_output = scale[1] * lax.dot_general(
        direction_all[1], right_rows, (((0,), (1,)), ((), ())), preferred_element_type=jnp.float32
    )
    query_new = query_master - 0.01 * step_query
    out_new = out_master - 0.01 * step_output
    query_copy, out_copy = (
        lax.all_gather(query_new.astype(jnp.bfloat16), "fs", axis=0, tiled=True),
        lax.all_gather(out_new.astype(jnp.bfloat16), "fs", axis=1, tiled=True),
    )
    return (query_new, out_new, query_copy, out_copy, first_new, second_new)


def choose_body(n_fs, n_tp, *args):
    left_factor, first_moment = args[4], args[8]
    model, part = left_factor.shape
    aligned = model % 128 == 0 and part % 16 == 0 and first_moment.shape[1] % 16 == 0
    aligned = aligned and first_moment.shape[2] % 128 == 0
    if aligned and n_fs % PAIR == 0 and n_tp % PAIR == 0:
        return fast_body(n_fs, n_tp, *args)
    return plain_body(*args)


def solution(mesh):
    return jax.shard_map(
        functools.partial(choose_body, mesh.shape["fs"], mesh.shape["tp"]),
        mesh=mesh,
        in_specs=(
            P("fs", None),
            P("fs", "tp"),
            P("fs", "tp"),
            P("fs", None),
            P("fs", "tp"),
            P("fs", "tp"),
            P("fs", "tp"),
            P("tp", "fs"),
            P(None, "fs", "tp"),
            P(None, "fs", "tp"),
        ),
        out_specs=(
            P("fs", "tp"),
            P("tp", "fs"),
            P(None, "tp"),
            P("tp", None),
            P(None, "fs", "tp"),
            P(None, "fs", "tp"),
        ),
        check_vma=False,
    )
```

```python
import functools

import jax
import jax.numpy as jnp
from jax import lax
from jax.experimental import pallas as pl
from jax.experimental.pallas import tpu as pltpu
from jax.sharding import PartitionSpec as P

MESH = pl.DeviceIdType.MESH
PAIR = 2
NT = (((1,), (1,)), ((), ()))
TN = (((0,), (0,)), ((), ()))


def moment_step(first, second, grads):
    first_next = 0.9 * first + 0.1 * grads
    second_next = 0.99 * second + 0.01 * grads * grads
    return (first_next, second_next, first_next / (jnp.sqrt(second_next) + 1e-08))


def rows(index, size):
    return pl.ds(pl.multiple_of(index * size, size), size)


def peer_along(axis, index):
    if axis == "fs":
        return (index, lax.axis_index("tp"))
    return (lax.axis_index("fs"), index)


class Gather:
    def __init__(self, axis, count, view, sems, own=None):
        self.axis, self.outer, self.view, self.sems = axis, count // PAIR, view, sems
        me = lax.axis_index(axis)
        self.high, self.low = me // PAIR, lax.rem(me, PAIR)
        self.own = view(me) if own is None else own
        self.me = me

    def copy(self, src, dst, stage, slot, target):
        return pltpu.make_async_remote_copy(
            src_ref=src,
            dst_ref=dst,
            send_sem=self.sems.at[stage, 0, slot],
            recv_sem=self.sems.at[stage, 1, slot],
            device_id=peer_along(self.axis, target),
            device_id_type=MESH,
        )

    def index(self, offset, low):
        return lax.rem(self.high + offset, self.outer) * PAIR + low

    def outward(self, offset):
        return self.copy(self.own, self.view(self.me), 0, offset, self.index(offset, self.low))

    def inward(self, offset):
        source = self.index(self.outer - offset, self.low)
        src = self.own if offset == 0 else self.view(source)
        partner = self.high * PAIR + 1 - self.low
        return self.copy(src, self.view(self.me if offset == 0 else source), 1, offset, partner)

    def start_outward(self):
        for offset in range(self.outer - 1, 0, -1):
            self.outward(offset).start()

    def start_inward(self):
        self.inward(0).start()

    def start(self):
        self.start_outward()
        self.start_inward()

    def forward(self):
        for offset in range(self.outer - 1, 0, -1):
            self.outward(offset).wait_recv()
            self.inward(offset).start()

    def finish(self):
        for offset in range(self.outer):
            self.inward(offset).wait_recv()
        for offset in range(1, self.outer):
            self.outward(offset).wait_send()
        for offset in range(self.outer):
            self.inward(offset).wait_send()


def kernel(
    n_fs,
    n_tp,
    saved_hbm,
    outcot_hbm,
    querycot_hbm,
    attn_hbm,
    query_hbm,
    out_hbm,
    factor_ref,
    first_ref,
    second_ref,
    query_out,
    out_out,
    query_copy,
    out_copy,
    first_out,
    second_out,
    factors_ref,
    dirs_ref,
    query_master,
    out_master,
    query_early,
    out_early,
    saved,
    outcot,
    querycot,
    attn,
    proj,
    grad,
    pair_send,
    pair_recv,
    far_send,
    far_recv,
    own_dir,
    square_buf,
    load_sems,
    factor_sems,
    proj_sems,
    columns_sems,
    pair_sems,
    far_sems,
    dir_sems,
    square_sems,
    early_sems,
    late_sems,
):
    me, column = lax.axis_index("fs"), lax.axis_index("tp")
    high, low = me // PAIR, lax.rem(me, PAIR)
    outer = n_fs // PAIR
    part = factor_ref.shape[1]
    width = factor_ref.shape[2]
    depth = first_ref.shape[1]
    loads = [
        pltpu.make_async_copy(src, dst, load_sems.at[i])
        for i, (src, dst) in enumerate(
            (
                (saved_hbm, saved),
                (outcot_hbm, outcot),
                (querycot_hbm, querycot),
                (attn_hbm, attn),
                (query_hbm, query_master),
                (out_hbm, out_master),
            )
        )
    ]
    for load in loads[4:] + loads[:4]:
        load.start()

    peers = [(lax.rem(high + i, outer) * PAIR + low, column) for i in range(1, outer)]
    peers.append((high * PAIR + 1 - low, column))
    peers += [(me, lax.rem(column + i, n_tp)) for i in range(1, n_tp)]
    barrier = pltpu.get_barrier_semaphore()
    for peer in peers:
        pl.semaphore_signal(barrier, inc=1, device_id=peer, device_id_type=MESH)
    pl.semaphore_wait(barrier, len(peers))

    factors = Gather(
        "fs",
        n_fs,
        lambda i: factors_ref.at[:, rows(column, part), rows(i, width)],
        factor_sems,
        own=factor_ref,
    )
    factors.start()
    factors_ref[:, rows(column, part), rows(me, width)] = factor_ref[...]

    half = query_copy.shape[1] // 2
    early = (
        Gather("fs", n_fs, lambda i: query_copy.at[rows(i, width), :half], early_sems.at[0], own=query_early),
        Gather("fs", n_fs, lambda i: out_copy.at[:half, rows(i, width)], early_sems.at[1], own=out_early),
    )
    loads[4].wait()
    query_early[...] = query_master[:, :half].astype(query_early.dtype)
    loads[5].wait()
    out_early[...] = out_master[:half, :].astype(out_early.dtype)
    for gather in early:
        gather.start_outward()
    factors.forward()
    for gather in early:
        gather.start_inward()
    factors.finish()

    gathers = []
    for k, tokens in enumerate((saved, outcot)):
        loads[k].wait()
        part_proj = lax.dot_general(
            factors_ref[k, rows(column, part), :],
            tokens[...],
            NT,
            preferred_element_type=jnp.float32,
        )
        proj[k, rows(column, part), :] = part_proj.astype(proj.dtype)
        gather = Gather(
            "tp", n_tp, lambda i, k=k: proj.at[k, rows(i, part), :], proj_sems.at[k]
        )
        gather.start()
        gathers.append(gather)
    columns = Gather("tp", n_tp, lambda i: factors_ref.at[:, rows(i, part), :], columns_sems)
    for gather in gathers:
        gather.forward()
    columns.start()
    for k, (gather, cot) in enumerate(zip(gathers, (querycot, attn))):
        gather.finish()
        loads[2 + k].wait()
        grad[k, :, :] = jnp.dot(proj[k], cot[...], preferred_element_type=jnp.float32)

    def pair_copy(offset):
        return pltpu.make_async_remote_copy(
            src_ref=pair_send.at[offset],
            dst_ref=pair_recv.at[offset],
            send_sem=pair_sems.at[0, offset],
            recv_sem=pair_sems.at[1, offset],
            device_id=(high * PAIR + 1 - low, column),
            device_id_type=MESH,
        )

    def far_copy(offset):
        return pltpu.make_async_remote_copy(
            src_ref=far_send.at[offset],
            dst_ref=far_recv.at[offset],
            send_sem=far_sems.at[0, offset],
            recv_sem=far_sems.at[1, offset],
            device_id=(lax.rem(high + offset, outer) * PAIR + low, column),
            device_id_type=MESH,
        )

    order = list(range(outer - 1, 0, -1)) + [0]
    for offset in order:
        target = lax.rem(high + offset, outer) * PAIR + 1 - low
        pair_send[offset] = grad[:, rows(target, depth), :].astype(pair_send.dtype)
        pair_copy(offset).start()
    for offset in order:
        target = lax.rem(high + offset, outer) * PAIR + low
        pair_copy(offset).wait_recv()
        both = grad[:, rows(target, depth), :] + pair_recv[offset].astype(jnp.float32)
        if offset:
            far_send[offset] = both.astype(far_send.dtype)
            far_copy(offset).start()
    total = both
    columns.forward()
    for gather in early:
        gather.forward()
    for offset in range(1, outer):
        far_copy(offset).wait_recv()
        total = total + far_recv[offset].astype(jnp.float32)

    first_new, second_new, direction = moment_step(first_ref[...], second_ref[...], total)
    own_dir[...] = direction.astype(own_dir.dtype)
    spread = Gather("fs", n_fs, lambda i: dirs_ref.at[:, rows(i, depth), :], dir_sems, own=own_dir)
    spread.start()
    dirs_ref[:, rows(me, depth), :] = own_dir[...]
    first_out[...] = first_new
    second_out[...] = second_new
    squares = direction * direction
    shape = square_buf.shape[1:]
    row = lax.broadcasted_iota(jnp.int32, shape, 0)
    mine = jnp.where(row == 0, jnp.sum(squares[0]), jnp.sum(squares[1]))

    rounds = (
        [(me, lax.rem(column + i, n_tp)) for i in range(1, n_tp)],
        [(lax.rem(high + i, outer) * PAIR + low, column) for i in range(1, outer)],
        [(high * PAIR + 1 - low, column)],
    )
    slot = 0
    tiny = []
    for stage, targets in enumerate(rounds):
        square_buf[slot] = mine
        base = slot
        copies = []
        for target in targets:
            slot += 1
            copies.append(
                pltpu.make_async_remote_copy(
                    src_ref=square_buf.at[base],
                    dst_ref=square_buf.at[slot],
                    send_sem=square_sems.at[0, slot],
                    recv_sem=square_sems.at[1, slot],
                    device_id=target,
                    device_id_type=MESH,
                )
            )
        for copy in copies:
            copy.start()
        if stage == 1:
            spread.forward()
        for i, copy in enumerate(copies):
            copy.wait_recv()
            mine = mine + square_buf[base + 1 + i]
        tiny += copies
        slot += 1
    spread.finish()
    columns.finish()

    entries = dirs_ref.shape[1] * dirs_ref.shape[2] * n_tp
    scale = 0.01 * lax.rsqrt(mine / entries + 1e-06)
    query_scale, out_scale = scale[0:1, 0:1], scale[1:2, 0:1]

    def step(k, block, part_of_features):
        factor = factors_ref[k, :, rows(block, width)]
        direction = dirs_ref[k, :, part_of_features]
        pair = (factor, direction) if k == 0 else (direction, factor)
        return lax.dot_general(*pair, TN, preferred_element_type=jnp.float32)

    late = (
        Gather("fs", n_fs, lambda i: query_copy.at[rows(i, width), half:], late_sems.at[0]),
        Gather("fs", n_fs, lambda i: out_copy.at[half:, rows(i, width)], late_sems.at[1]),
    )
    for part_of_features in (slice(half, None), slice(0, half)):
        query_new = query_master[:, part_of_features] - query_scale * step(0, me, part_of_features)
        query_out[:, part_of_features] = query_new
        query_copy[rows(me, width), part_of_features] = query_new.astype(query_copy.dtype)
        if part_of_features.start:
            late[0].start()
        out_new = out_master[part_of_features, :] - out_scale * step(1, me, part_of_features)
        out_out[part_of_features, :] = out_new
        out_copy[part_of_features, rows(me, width)] = out_new.astype(out_copy.dtype)
        if part_of_features.start:
            late[1].start()
    for gather in early:
        gather.finish()

    def finish_block(i, carry):
        block = lax.rem(me + i, n_fs)
        where = rows(block, width)
        query = query_copy[where, :half].astype(jnp.float32)
        query_copy[where, :half] = (query - query_scale * step(0, block, slice(0, half))).astype(query_copy.dtype)
        out = out_copy[:half, where].astype(jnp.float32)
        out_copy[:half, where] = (out - out_scale * step(1, block, slice(0, half))).astype(out_copy.dtype)
        return carry

    lax.fori_loop(1, n_fs, finish_block, 0)
    for gather in late:
        gather.forward()
    for gather in late:
        gather.finish()
    for offset in order:
        pair_copy(offset).wait_send()
        if offset:
            far_copy(offset).wait_send()
    for copy in tiny:
        copy.wait_send()


def fast_body(
    n_fs,
    n_tp,
    saved_inputs,
    query_cotangent,
    attn_outputs,
    out_cotangent,
    left_factor,
    right_factor,
    query_master,
    out_master,
    first_moment,
    second_moment,
):
    tokens, model = saved_inputs.shape
    features = query_cotangent.shape[1]
    width, part = left_factor.shape
    depth = first_moment.shape[1]
    rank = part * n_tp
    outer = n_fs // PAIR
    half = features // 2
    low, wide = jnp.bfloat16, jnp.float32
    vmem = pl.BlockSpec(memory_space=pltpu.VMEM)
    anywhere = pl.BlockSpec(memory_space=pl.ANY)
    dma = pltpu.SemaphoreType.DMA
    tiny_slots = n_tp + outer + PAIR
    factor = jnp.stack([left_factor.T, right_factor.T])
    return pl.pallas_call(
        functools.partial(kernel, n_fs, n_tp),
        out_shape=(
            jax.ShapeDtypeStruct((width, features), wide),
            jax.ShapeDtypeStruct((features, width), wide),
            jax.ShapeDtypeStruct((model, features), low),
            jax.ShapeDtypeStruct((features, model), low),
            jax.ShapeDtypeStruct(first_moment.shape, wide),
            jax.ShapeDtypeStruct(first_moment.shape, wide),
        ),
        in_specs=[anywhere] * 6 + [vmem] * 3,
        out_specs=(vmem,) * 6,
        scratch_shapes=[
            pltpu.VMEM((2, rank, model), low),
            pltpu.VMEM((2, rank, features), low),
            pltpu.VMEM((width, features), wide),
            pltpu.VMEM((features, width), wide),
            pltpu.VMEM((width, half), low),
            pltpu.VMEM((half, width), low),
            pltpu.VMEM((tokens, model), low),
            pltpu.VMEM((tokens, model), low),
            pltpu.VMEM((tokens, features), low),
            pltpu.VMEM((tokens, features), low),
            pltpu.VMEM((2, rank, tokens), low),
            pltpu.VMEM((2, rank, features), wide),
            pltpu.VMEM((outer, 2, depth, features), low),
            pltpu.VMEM((outer, 2, depth, features), low),
            pltpu.VMEM((outer, 2, depth, features), low),
            pltpu.VMEM((outer, 2, depth, features), low),
            pltpu.VMEM((2, depth, features), low),
            pltpu.VMEM((tiny_slots, 8, 128), wide),
            dma((6,)),
            dma((2, 2, outer)),
            dma((2, 2, 2, n_tp // PAIR)),
            dma((2, 2, n_tp // PAIR)),
            dma((2, outer)),
            dma((2, outer)),
            dma((2, 2, outer)),
            dma((2, tiny_slots)),
            dma((2, 2, 2, outer)),
            dma((2, 2, 2, outer)),
        ],
        compiler_params=pltpu.CompilerParams(
            collective_id=0, has_side_effects=True, vmem_limit_bytes=56 * 2**20
        ),
        cost_estimate=pl.CostEstimate(
            flops=4 * tokens * rank * (model + features), bytes_accessed=200 * 2**20, transcendentals=0
        ),
    )(
        saved_inputs,
        out_cotangent,
        query_cotangent,
        attn_outputs,
        query_master,
        out_master,
        factor,
        first_moment,
        second_moment,
    )


def plain_body(
    saved_inputs,
    query_cotangent,
    attn_outputs,
    out_cotangent,
    left_factor,
    right_factor,
    query_master,
    out_master,
    first_moment,
    second_moment,
):
    left_part = jnp.dot(
        saved_inputs,
        lax.all_gather(left_factor, "fs", axis=0, tiled=True),
        preferred_element_type=jnp.float32,
    )
    right_part = jnp.dot(
        out_cotangent,
        lax.all_gather(right_factor, "fs", axis=0, tiled=True),
        preferred_element_type=jnp.float32,
    )
    left_proj, right_proj, left_rows, right_rows = (
        lax.all_gather(left_part.astype(jnp.bfloat16), "tp", axis=1, tiled=True),
        lax.all_gather(right_part.astype(jnp.bfloat16), "tp", axis=1, tiled=True),
        lax.all_gather(left_factor, "tp", axis=1, tiled=True),
        lax.all_gather(right_factor, "tp", axis=1, tiled=True),
    )
    depth = first_moment.shape[1]
    grad_query = lax.dot_general(left_proj, query_cotangent, TN, preferred_element_type=jnp.float32)
    grad_output = lax.dot_general(right_proj, attn_outputs, TN, preferred_element_type=jnp.float32)
    summed = lax.psum_scatter(
        jnp.stack([grad_query, grad_output], axis=1), "fs", scatter_dimension=0, tiled=True
    )
    grads = jnp.transpose(summed, (1, 0, 2))
    first_new, second_new, own_direction = moment_step(first_moment, second_moment, grads)
    direction_all = lax.all_gather(own_direction.astype(jnp.bfloat16), "fs", axis=1, tiled=True)
    squares = jnp.sum(own_direction * own_direction, axis=(1, 2))
    total = lax.psum(squares, ("fs", "tp"))
    entries = depth * lax.axis_size("fs") * own_direction.shape[2] * lax.axis_size("tp")
    scale = lax.rsqrt(total / entries + 1e-06)
    step_query = scale[0] * jnp.dot(left_rows, direction_all[0], preferred_element_type=jnp.float32)
    step_output = scale[1] * lax.dot_general(
        direction_all[1], right_rows, (((0,), (1,)), ((), ())), preferred_element_type=jnp.float32
    )
    query_new = query_master - 0.01 * step_query
    out_new = out_master - 0.01 * step_output
    query_copy, out_copy = (
        lax.all_gather(query_new.astype(jnp.bfloat16), "fs", axis=0, tiled=True),
        lax.all_gather(out_new.astype(jnp.bfloat16), "fs", axis=1, tiled=True),
    )
    return (query_new, out_new, query_copy, out_copy, first_new, second_new)


def choose_body(n_fs, n_tp, *args):
    left_factor, first_moment = args[4], args[8]
    model, part = args[0].shape[1], left_factor.shape[1]
    aligned = part % 16 == 0 and first_moment.shape[1] % 16 == 0
    aligned = aligned and model // n_fs % 128 == 0 and first_moment.shape[2] % 256 == 0
    if aligned and n_fs % PAIR == 0 and n_tp % PAIR == 0:
        return fast_body(n_fs, n_tp, *args)
    return plain_body(*args)


def solution(mesh):
    return jax.shard_map(
        functools.partial(choose_body, mesh.shape["fs"], mesh.shape["tp"]),
        mesh=mesh,
        in_specs=(
            P("fs", None),
            P("fs", "tp"),
            P("fs", "tp"),
            P("fs", None),
            P("fs", "tp"),
            P("fs", "tp"),
            P("fs", "tp"),
            P("tp", "fs"),
            P(None, "fs", "tp"),
            P(None, "fs", "tp"),
        ),
        out_specs=(
            P("fs", "tp"),
            P("tp", "fs"),
            P(None, "tp"),
            P("tp", None),
            P(None, "fs", "tp"),
            P(None, "fs", "tp"),
        ),
        check_vma=False,
    )
```

```python
import functools

import jax
import jax.numpy as jnp
from jax import lax
from jax.experimental import pallas as pl
from jax.experimental.pallas import tpu as pltpu
from jax.sharding import PartitionSpec as P

MESH = pl.DeviceIdType.MESH
PAIR = 2
NT = (((1,), (1,)), ((), ()))
TN = (((0,), (0,)), ((), ()))


def moment_step(first, second, grads):
    first_next = 0.9 * first + 0.1 * grads
    second_next = 0.99 * second + 0.01 * grads * grads
    return (first_next, second_next, first_next / (jnp.sqrt(second_next) + 1e-08))


def rows(index, size):
    return pl.ds(pl.multiple_of(index * size, size), size)


def peer_along(axis, index):
    if axis == "fs":
        return (index, lax.axis_index("tp"))
    return (lax.axis_index("fs"), index)


class Gather:
    def __init__(self, axis, count, view, sems, own=None):
        self.axis, self.outer, self.view, self.sems = axis, count // PAIR, view, sems
        me = lax.axis_index(axis)
        self.high, self.low = me // PAIR, lax.rem(me, PAIR)
        self.own = view(me) if own is None else own
        self.me = me

    def copy(self, src, dst, stage, slot, target):
        return pltpu.make_async_remote_copy(
            src_ref=src,
            dst_ref=dst,
            send_sem=self.sems.at[stage, 0, slot],
            recv_sem=self.sems.at[stage, 1, slot],
            device_id=peer_along(self.axis, target),
            device_id_type=MESH,
        )

    def index(self, offset, low):
        return lax.rem(self.high + offset, self.outer) * PAIR + low

    def outward(self, offset):
        return self.copy(self.own, self.view(self.me), 0, offset, self.index(offset, self.low))

    def inward(self, offset):
        source = self.index(self.outer - offset, self.low)
        src = self.own if offset == 0 else self.view(source)
        partner = self.high * PAIR + 1 - self.low
        return self.copy(src, self.view(self.me if offset == 0 else source), 1, offset, partner)

    def start_outward(self):
        for offset in range(self.outer - 1, 0, -1):
            self.outward(offset).start()

    def start_inward(self):
        self.inward(0).start()

    def start(self):
        self.start_outward()
        self.start_inward()

    def forward(self):
        for offset in range(self.outer - 1, 0, -1):
            self.outward(offset).wait_recv()
            self.inward(offset).start()

    def finish(self):
        for offset in range(self.outer):
            self.inward(offset).wait_recv()
        for offset in range(1, self.outer):
            self.outward(offset).wait_send()
        for offset in range(self.outer):
            self.inward(offset).wait_send()


def kernel(
    n_fs,
    n_tp,
    saved_hbm,
    outcot_hbm,
    querycot_hbm,
    attn_hbm,
    query_hbm,
    out_hbm,
    factor_ref,
    first_ref,
    second_ref,
    query_out,
    out_out,
    query_copy,
    out_copy,
    first_out,
    second_out,
    factors_ref,
    dirs_ref,
    query_master,
    out_master,
    query_early,
    out_early,
    saved,
    outcot,
    querycot,
    attn,
    proj,
    grad,
    pair_send,
    pair_recv,
    far_send,
    far_recv,
    own_dir,
    square_buf,
    load_sems,
    factor_sems,
    proj_sems,
    columns_sems,
    pair_sems,
    far_sems,
    dir_sems,
    square_sems,
    early_sems,
    late_sems,
):
    me, column = lax.axis_index("fs"), lax.axis_index("tp")
    high, low = me // PAIR, lax.rem(me, PAIR)
    outer = n_fs // PAIR
    part = factor_ref.shape[1]
    width = factor_ref.shape[2]
    depth = first_ref.shape[1]
    loads = [
        pltpu.make_async_copy(src, dst, load_sems.at[i])
        for i, (src, dst) in enumerate(
            (
                (saved_hbm, saved),
                (outcot_hbm, outcot),
                (querycot_hbm, querycot),
                (attn_hbm, attn),
                (query_hbm, query_master),
                (out_hbm, out_master),
            )
        )
    ]
    for load in loads[4:] + loads[:4]:
        load.start()

    peers = [(lax.rem(high + i, outer) * PAIR + low, column) for i in range(1, outer)]
    peers.append((high * PAIR + 1 - low, column))
    peers += [(me, lax.rem(column + i, n_tp)) for i in range(1, n_tp)]
    barrier = pltpu.get_barrier_semaphore()
    for peer in peers:
        pl.semaphore_signal(barrier, inc=1, device_id=peer, device_id_type=MESH)
    pl.semaphore_wait(barrier, len(peers))

    factors = Gather(
        "fs",
        n_fs,
        lambda i: factors_ref.at[:, rows(column, part), rows(i, width)],
        factor_sems,
        own=factor_ref,
    )
    factors.start()
    factors_ref[:, rows(column, part), rows(me, width)] = factor_ref[...]

    half = query_copy.shape[1] // 2
    early = (
        Gather("fs", n_fs, lambda i: query_copy.at[rows(i, width), :half], early_sems.at[0], own=query_early),
        Gather("fs", n_fs, lambda i: out_copy.at[:half, rows(i, width)], early_sems.at[1], own=out_early),
    )
    loads[4].wait()
    query_early[...] = query_master[:, :half].astype(query_early.dtype)
    loads[5].wait()
    out_early[...] = out_master[:half, :].astype(out_early.dtype)
    for gather in early:
        gather.start_outward()
    factors.forward()
    for gather in early:
        gather.start_inward()
    factors.finish()

    gathers = []
    for k, tokens in enumerate((saved, outcot)):
        loads[k].wait()
        part_proj = lax.dot_general(
            factors_ref[k, rows(column, part), :],
            tokens[...],
            NT,
            preferred_element_type=jnp.float32,
        )
        proj[k, rows(column, part), :] = part_proj.astype(proj.dtype)
        gather = Gather(
            "tp", n_tp, lambda i, k=k: proj.at[k, rows(i, part), :], proj_sems.at[k]
        )
        gather.start()
        gathers.append(gather)
    columns = Gather("tp", n_tp, lambda i: factors_ref.at[:, rows(i, part), :], columns_sems)
    for gather in gathers:
        gather.forward()
    columns.start()
    for k, (gather, cot) in enumerate(zip(gathers, (querycot, attn))):
        gather.finish()
        loads[2 + k].wait()
        grad[k, :, :] = jnp.dot(proj[k], cot[...], preferred_element_type=jnp.float32)

    def pair_copy(offset):
        return pltpu.make_async_remote_copy(
            src_ref=pair_send.at[offset],
            dst_ref=pair_recv.at[offset],
            send_sem=pair_sems.at[0, offset],
            recv_sem=pair_sems.at[1, offset],
            device_id=(high * PAIR + 1 - low, column),
            device_id_type=MESH,
        )

    def far_copy(offset):
        return pltpu.make_async_remote_copy(
            src_ref=far_send.at[offset],
            dst_ref=far_recv.at[offset],
            send_sem=far_sems.at[0, offset],
            recv_sem=far_sems.at[1, offset],
            device_id=(lax.rem(high + offset, outer) * PAIR + low, column),
            device_id_type=MESH,
        )

    order = list(range(outer - 1, 0, -1)) + [0]
    for offset in order:
        target = lax.rem(high + offset, outer) * PAIR + 1 - low
        pair_send[offset] = grad[:, rows(target, depth), :].astype(pair_send.dtype)
        pair_copy(offset).start()
    for offset in order:
        target = lax.rem(high + offset, outer) * PAIR + low
        pair_copy(offset).wait_recv()
        both = grad[:, rows(target, depth), :] + pair_recv[offset].astype(jnp.float32)
        if offset:
            far_send[offset] = both.astype(far_send.dtype)
            far_copy(offset).start()
    total = both
    columns.forward()
    for gather in early:
        gather.forward()
    for offset in range(1, outer):
        far_copy(offset).wait_recv()
        total = total + far_recv[offset].astype(jnp.float32)

    first_new, second_new, direction = moment_step(first_ref[...], second_ref[...], total)
    own_dir[...] = direction.astype(own_dir.dtype)
    spread = Gather("fs", n_fs, lambda i: dirs_ref.at[:, rows(i, depth), :], dir_sems, own=own_dir)
    spread.start()
    dirs_ref[:, rows(me, depth), :] = own_dir[...]
    first_out[...] = first_new
    second_out[...] = second_new
    squares = direction * direction
    shape = square_buf.shape[1:]
    row = lax.broadcasted_iota(jnp.int32, shape, 0)
    mine = jnp.where(row == 0, jnp.sum(squares[0]), jnp.sum(squares[1]))

    rounds = (
        [(me, lax.rem(column + i, n_tp)) for i in range(1, n_tp)],
        [(lax.rem(high + i, outer) * PAIR + low, column) for i in range(1, outer)],
        [(high * PAIR + 1 - low, column)],
    )
    slot = 0
    tiny = []
    for stage, targets in enumerate(rounds):
        square_buf[slot] = mine
        base = slot
        copies = []
        for target in targets:
            slot += 1
            copies.append(
                pltpu.make_async_remote_copy(
                    src_ref=square_buf.at[base],
                    dst_ref=square_buf.at[slot],
                    send_sem=square_sems.at[0, slot],
                    recv_sem=square_sems.at[1, slot],
                    device_id=target,
                    device_id_type=MESH,
                )
            )
        for copy in copies:
            copy.start()
        if stage == 1:
            spread.forward()
        for i, copy in enumerate(copies):
            copy.wait_recv()
            mine = mine + square_buf[base + 1 + i]
        tiny += copies
        slot += 1
    spread.finish()
    columns.finish()

    entries = dirs_ref.shape[1] * dirs_ref.shape[2] * n_tp
    scale = 0.01 * lax.rsqrt(mine / entries + 1e-06)
    query_scale, out_scale = scale[0:1, 0:1], scale[1:2, 0:1]

    def step(k, block, part_of_features):
        factor = factors_ref[k, :, rows(block, width)]
        direction = dirs_ref[k, :, part_of_features]
        pair = (factor, direction) if k == 0 else (direction, factor)
        return lax.dot_general(*pair, TN, preferred_element_type=jnp.float32)

    tall, deep = width // 2, half // 2
    late_query = [
        Gather("fs", n_fs, lambda i, p=p: query_copy.at[rows(2 * i + p, tall), half:], late_sems.at[p])
        for p in range(2)
    ]
    late_out = [
        Gather(
            "fs",
            n_fs,
            lambda i, p=p: out_copy.at[half + p * deep : half + (p + 1) * deep, rows(i, width)],
            late_sems.at[2 + p],
        )
        for p in range(2)
    ]
    late = late_query + late_out
    for part_of_features in (slice(half, None), slice(0, half)):
        query_new = query_master[:, part_of_features] - query_scale * step(0, me, part_of_features)
        query_out[:, part_of_features] = query_new
        query_copy[rows(me, width), part_of_features] = query_new.astype(query_copy.dtype)
        if part_of_features.start:
            for gather in late_query:
                gather.start()
        out_new = out_master[part_of_features, :] - out_scale * step(1, me, part_of_features)
        out_out[part_of_features, :] = out_new
        out_copy[part_of_features, rows(me, width)] = out_new.astype(out_copy.dtype)
        if part_of_features.start:
            for gather in late_out:
                gather.start()
    for gather in early:
        gather.finish()

    def finish_block(i, carry):
        block = lax.rem(me + i, n_fs)
        where = rows(block, width)
        query = query_copy[where, :half].astype(jnp.float32)
        query_copy[where, :half] = (query - query_scale * step(0, block, slice(0, half))).astype(query_copy.dtype)
        out = out_copy[:half, where].astype(jnp.float32)
        out_copy[:half, where] = (out - out_scale * step(1, block, slice(0, half))).astype(out_copy.dtype)
        return carry

    lax.fori_loop(1, n_fs, finish_block, 0)
    for gather in late:
        gather.forward()
    for gather in late:
        gather.finish()
    for offset in order:
        pair_copy(offset).wait_send()
        if offset:
            far_copy(offset).wait_send()
    for copy in tiny:
        copy.wait_send()


def fast_body(
    n_fs,
    n_tp,
    saved_inputs,
    query_cotangent,
    attn_outputs,
    out_cotangent,
    left_factor,
    right_factor,
    query_master,
    out_master,
    first_moment,
    second_moment,
):
    tokens, model = saved_inputs.shape
    features = query_cotangent.shape[1]
    width, part = left_factor.shape
    depth = first_moment.shape[1]
    rank = part * n_tp
    outer = n_fs // PAIR
    half = features // 2
    low, wide = jnp.bfloat16, jnp.float32
    vmem = pl.BlockSpec(memory_space=pltpu.VMEM)
    anywhere = pl.BlockSpec(memory_space=pl.ANY)
    dma = pltpu.SemaphoreType.DMA
    tiny_slots = n_tp + outer + PAIR
    factor = jnp.stack([left_factor.T, right_factor.T])
    return pl.pallas_call(
        functools.partial(kernel, n_fs, n_tp),
        out_shape=(
            jax.ShapeDtypeStruct((width, features), wide),
            jax.ShapeDtypeStruct((features, width), wide),
            jax.ShapeDtypeStruct((model, features), low),
            jax.ShapeDtypeStruct((features, model), low),
            jax.ShapeDtypeStruct(first_moment.shape, wide),
            jax.ShapeDtypeStruct(first_moment.shape, wide),
        ),
        in_specs=[anywhere] * 6 + [vmem] * 3,
        out_specs=(vmem,) * 6,
        scratch_shapes=[
            pltpu.VMEM((2, rank, model), low),
            pltpu.VMEM((2, rank, features), low),
            pltpu.VMEM((width, features), wide),
            pltpu.VMEM((features, width), wide),
            pltpu.VMEM((width, half), low),
            pltpu.VMEM((half, width), low),
            pltpu.VMEM((tokens, model), low),
            pltpu.VMEM((tokens, model), low),
            pltpu.VMEM((tokens, features), low),
            pltpu.VMEM((tokens, features), low),
            pltpu.VMEM((2, rank, tokens), low),
            pltpu.VMEM((2, rank, features), wide),
            pltpu.VMEM((outer, 2, depth, features), low),
            pltpu.VMEM((outer, 2, depth, features), low),
            pltpu.VMEM((outer, 2, depth, features), low),
            pltpu.VMEM((outer, 2, depth, features), low),
            pltpu.VMEM((2, depth, features), low),
            pltpu.VMEM((tiny_slots, 8, 128), wide),
            dma((6,)),
            dma((2, 2, outer)),
            dma((2, 2, 2, n_tp // PAIR)),
            dma((2, 2, n_tp // PAIR)),
            dma((2, outer)),
            dma((2, outer)),
            dma((2, 2, outer)),
            dma((2, tiny_slots)),
            dma((2, 2, 2, outer)),
            dma((4, 2, 2, outer)),
        ],
        compiler_params=pltpu.CompilerParams(
            collective_id=0, has_side_effects=True, vmem_limit_bytes=56 * 2**20
        ),
        cost_estimate=pl.CostEstimate(
            flops=4 * tokens * rank * (model + features), bytes_accessed=200 * 2**20, transcendentals=0
        ),
    )(
        saved_inputs,
        out_cotangent,
        query_cotangent,
        attn_outputs,
        query_master,
        out_master,
        factor,
        first_moment,
        second_moment,
    )


def plain_body(
    saved_inputs,
    query_cotangent,
    attn_outputs,
    out_cotangent,
    left_factor,
    right_factor,
    query_master,
    out_master,
    first_moment,
    second_moment,
):
    left_part = jnp.dot(
        saved_inputs,
        lax.all_gather(left_factor, "fs", axis=0, tiled=True),
        preferred_element_type=jnp.float32,
    )
    right_part = jnp.dot(
        out_cotangent,
        lax.all_gather(right_factor, "fs", axis=0, tiled=True),
        preferred_element_type=jnp.float32,
    )
    left_proj, right_proj, left_rows, right_rows = (
        lax.all_gather(left_part.astype(jnp.bfloat16), "tp", axis=1, tiled=True),
        lax.all_gather(right_part.astype(jnp.bfloat16), "tp", axis=1, tiled=True),
        lax.all_gather(left_factor, "tp", axis=1, tiled=True),
        lax.all_gather(right_factor, "tp", axis=1, tiled=True),
    )
    depth = first_moment.shape[1]
    grad_query = lax.dot_general(left_proj, query_cotangent, TN, preferred_element_type=jnp.float32)
    grad_output = lax.dot_general(right_proj, attn_outputs, TN, preferred_element_type=jnp.float32)
    summed = lax.psum_scatter(
        jnp.stack([grad_query, grad_output], axis=1), "fs", scatter_dimension=0, tiled=True
    )
    grads = jnp.transpose(summed, (1, 0, 2))
    first_new, second_new, own_direction = moment_step(first_moment, second_moment, grads)
    direction_all = lax.all_gather(own_direction.astype(jnp.bfloat16), "fs", axis=1, tiled=True)
    squares = jnp.sum(own_direction * own_direction, axis=(1, 2))
    total = lax.psum(squares, ("fs", "tp"))
    entries = depth * lax.axis_size("fs") * own_direction.shape[2] * lax.axis_size("tp")
    scale = lax.rsqrt(total / entries + 1e-06)
    step_query = scale[0] * jnp.dot(left_rows, direction_all[0], preferred_element_type=jnp.float32)
    step_output = scale[1] * lax.dot_general(
        direction_all[1], right_rows, (((0,), (1,)), ((), ())), preferred_element_type=jnp.float32
    )
    query_new = query_master - 0.01 * step_query
    out_new = out_master - 0.01 * step_output
    query_copy, out_copy = (
        lax.all_gather(query_new.astype(jnp.bfloat16), "fs", axis=0, tiled=True),
        lax.all_gather(out_new.astype(jnp.bfloat16), "fs", axis=1, tiled=True),
    )
    return (query_new, out_new, query_copy, out_copy, first_new, second_new)


def choose_body(n_fs, n_tp, *args):
    left_factor, first_moment = args[4], args[8]
    model, part = args[0].shape[1], left_factor.shape[1]
    aligned = part % 16 == 0 and first_moment.shape[1] % 16 == 0
    aligned = aligned and model // n_fs % 128 == 0 and first_moment.shape[2] % 256 == 0
    aligned = aligned and model // n_fs % 32 == 0 and first_moment.shape[2] % 64 == 0
    if aligned and n_fs % PAIR == 0 and n_tp % PAIR == 0:
        return fast_body(n_fs, n_tp, *args)
    return plain_body(*args)


def solution(mesh):
    return jax.shard_map(
        functools.partial(choose_body, mesh.shape["fs"], mesh.shape["tp"]),
        mesh=mesh,
        in_specs=(
            P("fs", None),
            P("fs", "tp"),
            P("fs", "tp"),
            P("fs", None),
            P("fs", "tp"),
            P("fs", "tp"),
            P("fs", "tp"),
            P("tp", "fs"),
            P(None, "fs", "tp"),
            P(None, "fs", "tp"),
        ),
        out_specs=(
            P("fs", "tp"),
            P("tp", "fs"),
            P(None, "tp"),
            P("tp", None),
            P(None, "fs", "tp"),
            P(None, "fs", "tp"),
        ),
        check_vma=False,
    )
```
